32 devices in a mesh: ep: 8 (over z, x), tp: 4 (over y, core).
Axes of the slice: x: 2, y: 2, z: 4, core: 2. Of those that a mesh axis runs over, the one named last changes fastest.
Arguments:
- mixer_input: bfloat16 [1024, 2048], P('ep'), may hold values from -6 to 6
- mixer_gain: bfloat16 [2048], replicated, may hold values from 0.099609375 to 1.8984375
- query_matrix: bfloat16 [2048, 2048], P(None, 'tp'), may hold values from -0.125 to 0.125
- key_matrix: bfloat16 [2048, 2048], P(None, 'tp'), may hold values from -0.125 to 0.125
- value_matrix: bfloat16 [2048, 2048], P(None, 'tp'), may hold values from -0.125 to 0.125
- decay_down_factor: bfloat16 [2048, 64], replicated, may hold values from -0.125 to 0.125
- decay_up_factor: bfloat16 [64, 2048], P(None, 'tp'), may hold values from -1.1953125 to 1.1953125
- decay_bias_base: float32 [2048], P('tp'), may hold values from -16 to 0
- decay_shift: float32 [1024, 2048], P('ep', 'tp'), may hold values from -1.5 to 1.5
- decay_spike: float32 [1024, 2048], P('ep', 'tp'), may hold values from -1.4 to 0
- correction_rate_down: bfloat16 [2048, 64], replicated, may hold values from -0.125 to 0.125
- correction_rate_up: bfloat16 [64, 2048], P(None, 'tp'), may hold values from -1.1953125 to 1.1953125
- correction_rate_base: float32 [2048], P('tp'), may hold values from -8 to 1
- head_norm_gain: bfloat16 [2048], P('tp'), may hold values from 0.099609375 to 1.8984375
- output_weight: bfloat16 [2048, 2048], P('tp'), may hold values from -0.125 to 0.125
- feedforward_input: bfloat16 [2048, 2048], P(('ep', 'tp')), may hold values from -6 to 6
- feedforward_gain: bfloat16 [2048], replicated, may hold values from 0.099609375 to 1.8984375
- routed_expert_index: int32 [2048, 2], P('ep'), may hold values from 0 to 15, all different within a row; in each aligned block of 64 rows (0 to 63, 64 to 127, ...) at most 12 rows name the same one
- routed_expert_weight: float32 [2048, 2], P(('ep', 'tp')), may hold values from 0.3 to 2.5
- expert_gate_weight: bfloat16 [16, 2048, 1024], P('ep', None, 'tp'), may hold values from -0.125 to 0.125
- expert_up_weight: bfloat16 [16, 2048, 1024], P('ep', None, 'tp'), may hold values from -0.125 to 0.125
- expert_down_weight: bfloat16 [16, 1024, 2048], P('ep', 'tp'), may hold values from -0.1875 to 0.1875
- shared_gate_weight: bfloat16 [2048, 1024], P(None, 'tp'), may hold values from -0.125 to 0.125
- shared_up_weight: bfloat16 [2048, 1024], P(None, 'tp'), may hold values from -0.125 to 0.125
- shared_down_weight: bfloat16 [1024, 2048], P('tp'), may hold values from -0.1875 to 0.1875
Outputs:
- mixed_a: bfloat16 [1024, 2048], P(('ep', 'tp'))
- mixed_b: bfloat16 [2048, 2048], P(('ep', 'tp'))
The draws below stay inside these ranges and needn't reach their ends.
Inputs may be any that keep to these rules, and one draw needn't show every extreme that they name: `routed_expert_index`: in each aligned block of 64 rows (the rows of one device) a row names 2 different experts and no expert is named more than 12 times; in every draw some block names some expert exactly 12 times.
All inputs are finite; a program needn't handle non-finite values.
Results may differ from the reference program's by a relative error of at most 0.017.
Values may be sent and summed in bfloat16 or wider, within the bound.
A program may use at most 128 MiB of HBM per device.

```python
import math
import jax
import jax.numpy as jnp
import numpy as np
from jax import lax

MODEL_DIMENSION = 2048
MIXER_HEADS = 32
HEAD = 64
DECAY_RANK = 64
FE = 1024
TOP = 2
SPAN = 32
ROWS_A = 128
MIXER_CHANNELS = 2048
EXPERTS = 16
TOKB = 64
CAP = 12
FIRST_TOKENS = 1024
TOKENS_B = 2048
N_EP = 8
N_TP = 4


def slow_heads(key):
    shuffled = jax.random.permutation(jax.random.fold_in(key, 11), MIXER_HEADS)
    keep_count = MIXER_HEADS // 2
    return jnp.repeat(shuffled < keep_count, HEAD)


def draw_decay_bias_base(key, part):
    slow = slow_heads(key)
    noise = jax.random.uniform(jax.random.fold_in(key, 1), (MIXER_HEADS * HEAD,), jnp.float32, -0.5, 0.5)
    slow_level = math.log(0.3 / FIRST_TOKENS) + 0.5
    fast_level = math.log(1.0 / 40.0) + 0.5
    return jnp.where(slow, slow_level, fast_level) + noise


def draw_correction_rate_base(key, part):
    slow = slow_heads(key)
    noise = jax.random.uniform(jax.random.fold_in(key, 2), (MIXER_HEADS * HEAD,), jnp.float32, -0.5, 0.5)
    return jnp.where(slow, -7.0 + noise, 2.0 * noise)


def draw_decay_shift(key, part):
    channel_count = MIXER_HEADS * HEAD
    segments = FIRST_TOKENS // ROWS_A
    spans = FIRST_TOKENS // SPAN
    coarse = jax.random.uniform(jax.random.fold_in(key, 3), (segments, channel_count), jnp.float32, -0.7, 0.7)
    detail = jax.random.uniform(jax.random.fold_in(key, 4), (spans, channel_count), jnp.float32, -0.4, 0.4)
    return jnp.repeat(coarse, ROWS_A, axis=0) + jnp.repeat(detail, SPAN, axis=0)


def draw_decay_spike(key, part):
    channel_count = MIXER_HEADS * HEAD
    spike_count = 6
    slot_places = jax.random.randint(jax.random.fold_in(key, 5), (spike_count, MIXER_HEADS), 0, FIRST_TOKENS)
    layer_depth = jax.random.uniform(jax.random.fold_in(key, 6), (spike_count, channel_count), jnp.float32, math.log(0.5), math.log(0.8))
    positions = jnp.arange(FIRST_TOKENS, dtype=jnp.int32)
    result = jnp.zeros((FIRST_TOKENS, channel_count), jnp.float32)
    for item_number in range(spike_count):
        hits = (positions[:, None] == jnp.repeat(slot_places[item_number], HEAD)[None, :]).astype(jnp.float32)
        result = result + hits * layer_depth[item_number][None, :]
    return result


def level_of(key, shape, shards, smallest, top_value):
    factor_of = 1.0
    for axis_at, shards_of in shards:
        heights = jax.random.uniform(jax.random.fold_in(jax.random.fold_in(key, 6), axis_at), (shards_of,), jnp.float32, smallest / len(shards), top_value / len(shards))
        factor_of = factor_of * jnp.repeat(jnp.exp(heights), shape[axis_at] // shards_of).reshape((-1,) + (1,) * (len(shape) - 1 - axis_at))
    return factor_of


def deal_out(own_key, own, number, rows, amount, top, limit, slope):
    order = jax.random.permutation(own_key, amount)
    crowded, ordinary = portions_of(amount, rows * top, limit, slope, True), portions_of(amount, rows * top, limit, slope, False)
    places = jnp.arange(amount)

    def named(lengths, rotation):
        used = int((lengths > 0).sum())
        fixed = max(1, used // 4)
        shifted = fixed + (places - fixed + rotation * (used - fixed)) % max(1, amount - fixed)
        return jnp.zeros((amount,), jnp.int32).at[order[jnp.where(places < fixed, places, shifted)]].set(jnp.asarray(lengths, jnp.int32))

    lengths = jnp.where(number % 4 == 0, named(crowded, number // 4), named(ordinary, number - number // 4 - 1))
    mixed = jax.random.permutation(jax.random.fold_in(own, 3), amount)
    giver, taker = mixed[0:amount // 2 * 2:2], mixed[1:amount // 2 * 2:2]
    margin = jnp.minimum(lengths[giver] - 1, limit - lengths[taker]) // 2
    margin = jnp.where((giver == order[0]) | (taker == order[0]) | (lengths[taker] == 0), 0, jnp.maximum(margin, 0))
    shifted = jax.random.randint(jax.random.fold_in(own, 4), (amount // 2,), 0, 1 << 20) % (margin + 1)
    lengths = lengths.at[giver].add(-shifted).at[taker].add(shifted)
    labels = jnp.searchsorted(jnp.cumsum(lengths), jnp.arange(rows * top), side="right").astype(jnp.int32)
    table = labels.reshape(top, rows).T
    table = table[jax.random.permutation(jax.random.fold_in(own, 1), rows)]
    rotation = jax.random.randint(jax.random.fold_in(own, 2), (rows, 1), 0, top)
    return jnp.take_along_axis(table, (jnp.arange(top)[None, :] + rotation) % top, axis=1)


def portions_of(count, total, limit, lean, full):
    loads = [(1 << 20) // math.isqrt(rank ** lean) + 1 for rank in range(1, count + 1)]
    largest = limit if full else min(limit, max(-(-total // count), total * loads[0] // sum(loads)))
    least = 1 if total - largest >= count - 1 else 0
    holding, surplus = [largest] + [least] * (count - 1), total - largest - least * (count - 1)
    while surplus > 0:
        movable = [i for i in range(1, count) if holding[i] < largest] or [i for i in range(1, count) if holding[i] < limit]
        mass, left = sum([loads[i] for i in movable]), surplus
        for i in movable:
            addition = min(limit - holding[i], max(1, left * loads[i] // mass), surplus)
            holding[i] = holding[i] + addition
            surplus = surplus - addition
    return np.array(holding)


def scatter_about(rng, extent, spread, bound, split=(), kind=jnp.bfloat16):
    factor_of = level_of(rng, extent, split, -0.22, 0.18) if split else 1.0
    values = jax.random.normal(rng, extent, jnp.float32) * spread * factor_of
    return jnp.minimum(jnp.maximum(values, -bound), bound).astype(kind)


def setup_inputs(seed: int = 0) -> dict:
    arg_keys = jax.random.split(jax.random.key(seed), 26)
    mixer_input = scatter_about(arg_keys[0], (FIRST_TOKENS, MODEL_DIMENSION), 1.0, 6.0, ((0, 8),))
    mixer_gain = jnp.clip(1.0 + 0.18 * jax.random.normal(arg_keys[1], (MODEL_DIMENSION,), jnp.float32), 0.099609375, 1.8984375).astype(jnp.bfloat16)
    query_matrix = scatter_about(arg_keys[2], (MODEL_DIMENSION, MIXER_CHANNELS), MODEL_DIMENSION ** -0.5, 0.125, ((1, 4),))
    key_matrix = scatter_about(arg_keys[3], (MODEL_DIMENSION, MIXER_CHANNELS), MODEL_DIMENSION ** -0.5, 0.125, ((1, 4),))
    value_matrix = scatter_about(arg_keys[4], (MODEL_DIMENSION, MIXER_CHANNELS), MODEL_DIMENSION ** -0.5, 0.125, ((1, 4),))
    decay_down_factor = scatter_about(arg_keys[5], (MODEL_DIMENSION, DECAY_RANK), MODEL_DIMENSION ** -0.5, 0.125)
    decay_up_factor = scatter_about(arg_keys[6], (DECAY_RANK, MIXER_CHANNELS), 0.2, 1.1953125, ((1, 4),))
    decay_bias_base = draw_decay_bias_base(jax.random.fold_in(arg_keys[25], 71), 0)
    decay_shift = draw_decay_shift(jax.random.fold_in(arg_keys[25], 71), 0)
    decay_spike = draw_decay_spike(jax.random.fold_in(arg_keys[25], 71), 0)
    correction_rate_down = scatter_about(arg_keys[10], (MODEL_DIMENSION, DECAY_RANK), MODEL_DIMENSION ** -0.5, 0.125)
    correction_rate_up = scatter_about(arg_keys[11], (DECAY_RANK, MIXER_CHANNELS), 0.2, 1.1953125, ((1, 4),))
    correction_rate_base = draw_correction_rate_base(jax.random.fold_in(arg_keys[25], 71), 0)
    head_norm_gain = jnp.clip(1.0 + 0.18 * jax.random.normal(arg_keys[13], (MIXER_CHANNELS,), jnp.float32), 0.099609375, 1.8984375).astype(jnp.bfloat16)
    output_weight = scatter_about(arg_keys[14], (MIXER_CHANNELS, MODEL_DIMENSION), MIXER_CHANNELS ** -0.5, 0.125, ((0, 4),))
    feedforward_input = scatter_about(arg_keys[15], (TOKENS_B, MODEL_DIMENSION), 1.0, 6.0, ((0, 32),))
    feedforward_gain = jnp.clip(1.0 + 0.18 * jax.random.normal(arg_keys[16], (MODEL_DIMENSION,), jnp.float32), 0.099609375, 1.8984375).astype(jnp.bfloat16)
    routed_expert_index_keys = jax.random.split(jax.random.fold_in(arg_keys[17], 1), TOKENS_B // TOKB)
    routed_expert_index_turns = jax.random.permutation(jax.random.fold_in(arg_keys[17], 3), TOKENS_B // TOKB)
    routed_expert_index = jax.vmap(lambda own, number: deal_out(jax.random.fold_in(arg_keys[17], 2), own, number, TOKB, EXPERTS, TOP, CAP, 1))(routed_expert_index_keys, routed_expert_index_turns).reshape((TOKENS_B, TOP))
    routed_expert_weight = jnp.clip(jnp.exp(math.log(2.5) - 2.1202635 * jax.random.uniform(arg_keys[18], (TOKENS_B, TOP), jnp.float32) ** level_of(arg_keys[18], (TOKENS_B, TOP), ((0, 32),), -0.2, 0.2)), 0.3, 2.5)
    expert_gate_weight = scatter_about(arg_keys[19], (EXPERTS, MODEL_DIMENSION, FE), MODEL_DIMENSION ** -0.5, 0.125, ((0, 8), (2, 4)))
    expert_up_weight = scatter_about(arg_keys[20], (EXPERTS, MODEL_DIMENSION, FE), MODEL_DIMENSION ** -0.5, 0.125, ((0, 8), (2, 4)))
    expert_down_weight = scatter_about(arg_keys[21], (EXPERTS, FE, MODEL_DIMENSION), FE ** -0.5, 0.1875, ((0, 8), (1, 4)))
    shared_gate_weight = scatter_about(arg_keys[22], (MODEL_DIMENSION, FE), MODEL_DIMENSION ** -0.5, 0.125, ((1, 4),))
    shared_up_weight = scatter_about(arg_keys[23], (MODEL_DIMENSION, FE), MODEL_DIMENSION ** -0.5, 0.125, ((1, 4),))
    shared_down_weight = scatter_about(arg_keys[24], (FE, MODEL_DIMENSION), FE ** -0.5, 0.1875, ((0, 4),))
    return {"mixer_input": mixer_input, "mixer_gain": mixer_gain, "query_matrix": query_matrix, "key_matrix": key_matrix, "value_matrix": value_matrix, "decay_down_factor": decay_down_factor, "decay_up_factor": decay_up_factor, "decay_bias_base": decay_bias_base, "decay_shift": decay_shift, "decay_spike": decay_spike, "correction_rate_down": correction_rate_down, "correction_rate_up": correction_rate_up, "correction_rate_base": correction_rate_base, "head_norm_gain": head_norm_gain, "output_weight": output_weight, "feedforward_input": feedforward_input, "feedforward_gain": feedforward_gain, "routed_expert_index": routed_expert_index, "routed_expert_weight": routed_expert_weight, "expert_gate_weight": expert_gate_weight, "expert_up_weight": expert_up_weight, "expert_down_weight": expert_down_weight, "shared_gate_weight": shared_gate_weight, "shared_up_weight": shared_up_weight, "shared_down_weight": shared_down_weight}


highest = lax.Precision.HIGHEST
norm_eps = 1e-06
group_eps = 0.00064
unit_eps = 1e-06

def rms_rows(matrix, gain):
    values = matrix.astype(jnp.float32)
    scaled = values * lax.rsqrt(lax.optimization_barrier(jnp.mean(values * values, axis=-1, keepdims=True)) + norm_eps)
    return (scaled * gain.astype(jnp.float32)).astype(jnp.bfloat16)

def mixer_channel_rows(normed_rows, query_matrix, key_matrix, value_matrix, decay_down_factor, decay_up_factor, decay_bias_base, decay_shift, decay_spike, correction_rate_down, correction_rate_up, correction_rate_base):
    row_count = normed_rows.shape[0]
    head_count = query_matrix.shape[1] // HEAD

    def by_heads(matrix):
        return matrix.reshape(row_count, head_count, HEAD)
    query_matrix_rows = jnp.dot(normed_rows, query_matrix, preferred_element_type=jnp.float32)
    key_matrix_rows = jnp.dot(normed_rows, key_matrix, preferred_element_type=jnp.float32)
    value_matrix_rows = jnp.dot(normed_rows, value_matrix, preferred_element_type=jnp.float32)
    decay_low = jnp.tanh(jnp.dot(normed_rows, decay_down_factor, preferred_element_type=jnp.float32)).astype(jnp.bfloat16)
    decay_logits = decay_bias_base + jnp.dot(decay_low, decay_up_factor, preferred_element_type=jnp.float32) + decay_shift
    logarithm_decay = decay_spike - jnp.exp(-jax.nn.softplus(-decay_logits) - 0.5)
    iclr_low = jnp.dot(normed_rows, correction_rate_down, preferred_element_type=jnp.float32).astype(jnp.bfloat16)
    learning = jax.nn.sigmoid(correction_rate_base + jnp.dot(iclr_low, correction_rate_up, preferred_element_type=jnp.float32))
    key_matrix_rows = by_heads(key_matrix_rows)
    unit_keys = key_matrix_rows * lax.rsqrt(lax.optimization_barrier(jnp.sum(key_matrix_rows * key_matrix_rows, axis=-1, keepdims=True)) + unit_eps)
    return (by_heads(query_matrix_rows), key_matrix_rows, by_heads(value_matrix_rows), -unit_keys, unit_keys * by_heads(learning), by_heads(logarithm_decay))

def head_norm(outputs, gain):
    row_mean = lax.optimization_barrier(jnp.mean(outputs, axis=-1, keepdims=True))
    centered = outputs - row_mean
    row_var = lax.optimization_barrier(jnp.mean(centered * centered, axis=-1, keepdims=True))
    scaled = (centered * lax.rsqrt(row_var + group_eps)).reshape(outputs.shape[0], -1)
    return (scaled * gain.astype(jnp.float32)).astype(jnp.bfloat16)

def reference(mixer_input, mixer_gain, query_matrix, key_matrix, value_matrix, decay_down_factor, decay_up_factor, decay_bias_base, decay_shift, decay_spike, correction_rate_down, correction_rate_up, correction_rate_base, head_norm_gain, output_weight, feedforward_input, feedforward_gain, routed_expert_index, routed_expert_weight, expert_gate_weight, expert_up_weight, expert_down_weight, shared_gate_weight, shared_up_weight, shared_down_weight):
    normed_first = rms_rows(mixer_input, mixer_gain)
    query_matrix_rows, key_matrix_rows, value_matrix_rows, erase_vector, write_vector, logarithm_decay = mixer_channel_rows(normed_first, query_matrix, key_matrix, value_matrix, decay_down_factor, decay_up_factor, decay_bias_base, decay_shift, decay_spike, correction_rate_down, correction_rate_up, correction_rate_base)
    head_count = query_matrix_rows.shape[1]

    def advance(carried, inputs):
        query_t, key_t, value_t, erase_t, write_t, decay_t = inputs
        held = jnp.einsum('hvk,hk->hv', carried, erase_t, precision=highest)
        carried = carried * jnp.exp(decay_t)[:, None, :] + held[:, :, None] * write_t[:, None, :] + value_t[:, :, None] * key_t[:, None, :]
        return (carried, jnp.einsum('hvk,hk->hv', carried, query_t, precision=highest))
    initial = jnp.zeros((head_count, HEAD, HEAD), jnp.float32)
    _, head_out = lax.scan(advance, initial, (query_matrix_rows, key_matrix_rows, value_matrix_rows, erase_vector, write_vector, logarithm_decay))
    mixed_rows = head_norm(head_out, head_norm_gain)
    mixed_a = jnp.dot(mixed_rows, output_weight, preferred_element_type=jnp.float32).astype(jnp.bfloat16)
    normed_b = rms_rows(feedforward_input, feedforward_gain)
    total = normed_b.shape[0]
    model_width = normed_b.shape[1]
    padded = jnp.concatenate([normed_b, jnp.zeros((1, model_width), jnp.bfloat16)], axis=0)
    flat_ids = routed_expert_index.reshape(-1)
    most = N_EP * N_TP * CAP
    slice_width = FE // N_TP

    def one_expert(expert):
        picked = jnp.nonzero(flat_ids == expert, size=most, fill_value=total * TOP)[0].astype(jnp.int32)
        chosen = padded[picked // TOP]
        gate_out = jnp.dot(chosen, expert_gate_weight[expert], preferred_element_type=jnp.float32)
        up_out = jnp.dot(chosen, expert_up_weight[expert], preferred_element_type=jnp.float32)
        hidden = (jax.nn.silu(gate_out) * up_out).astype(jnp.bfloat16)
        pieces = hidden.astype(jnp.float32).reshape(most, N_TP, slice_width)
        down_blocks = expert_down_weight[expert].astype(jnp.float32).reshape(N_TP, slice_width, model_width)
        partial_value = jnp.einsum('rtf,tfd->trd', pieces, down_blocks)
        rounded = lax.optimization_barrier(partial_value.astype(jnp.bfloat16))
        summed = lax.optimization_barrier(jnp.sum(rounded.astype(jnp.float32), axis=0))
        return (summed.astype(jnp.bfloat16), picked)
    expert_out, picks = lax.map(one_expert, jnp.arange(EXPERTS, dtype=jnp.int32))
    placed = jnp.zeros((total * TOP + 1, model_width), jnp.bfloat16)
    placed = placed.at[picks.reshape(-1)].set(expert_out.reshape(-1, model_width))
    per_choice = placed[:total * TOP].reshape(total, TOP, model_width).astype(jnp.float32)
    routed = jnp.einsum('rk,rkd->rd', routed_expert_weight, per_choice, precision=highest)
    shared_hidden = (jax.nn.silu(jnp.dot(normed_b, shared_gate_weight, preferred_element_type=jnp.float32)) * jnp.dot(normed_b, shared_up_weight, preferred_element_type=jnp.float32)).astype(jnp.bfloat16)
    shared = jnp.zeros((total, model_width), jnp.float32)
    for block in range(N_TP):
        partial_value = jnp.dot(shared_hidden[:, block * slice_width:(block + 1) * slice_width], shared_down_weight[block * slice_width:(block + 1) * slice_width], preferred_element_type=jnp.float32)
        shared = shared + lax.optimization_barrier(partial_value.astype(jnp.bfloat16)).astype(jnp.float32)
    mixed_b = (routed + shared).astype(jnp.bfloat16)
    return (mixed_a, mixed_b)
```

```python
import jax
import jax.numpy as jnp
from jax import lax
from jax.experimental import pallas as pl
from jax.experimental.pallas import tpu as pltpu
from jax.sharding import PartitionSpec as P

HEAD = 64
TOP = 2
CHUNK = 64
PAIR = 2


highest = lax.Precision.HIGHEST
norm_eps = 1e-06
group_eps = 0.00064
unit_eps = 1e-06


def rms_rows(matrix, gain):
    values = matrix.astype(jnp.float32)
    scaled = values * lax.rsqrt(jnp.mean(values * values, axis=-1, keepdims=True) + norm_eps)
    return (scaled * gain.astype(jnp.float32)).astype(jnp.bfloat16)


def mixer_channel_rows(
    normed_rows,
    query_matrix,
    key_matrix,
    value_matrix,
    decay_down_factor,
    decay_up_factor,
    decay_bias_base,
    decay_shift,
    decay_spike,
    correction_rate_down,
    correction_rate_up,
    correction_rate_base,
):
    query_matrix_rows = jnp.dot(normed_rows, query_matrix, preferred_element_type=jnp.float32)
    key_matrix_rows = jnp.dot(normed_rows, key_matrix, preferred_element_type=jnp.float32)
    value_matrix_rows = jnp.dot(normed_rows, value_matrix, preferred_element_type=jnp.float32)
    decay_low = jnp.tanh(
        jnp.dot(normed_rows, decay_down_factor, preferred_element_type=jnp.float32)
    ).astype(jnp.bfloat16)
    decay_logits = (
        decay_bias_base
        + jnp.dot(decay_low, decay_up_factor, preferred_element_type=jnp.float32)
        + decay_shift
    )
    logarithm_decay = decay_spike - jnp.exp(-jax.nn.softplus(-decay_logits) - 0.5)
    iclr_low = jnp.dot(
        normed_rows, correction_rate_down, preferred_element_type=jnp.float32
    ).astype(jnp.bfloat16)
    learning = jax.nn.sigmoid(
        correction_rate_base
        + jnp.dot(iclr_low, correction_rate_up, preferred_element_type=jnp.float32)
    )
    return (query_matrix_rows, key_matrix_rows, value_matrix_rows, logarithm_decay, learning)


def dot_nn(left, right):
    return lax.dot_general(
        left, right, (((1,), (0,)), ((), ())), preferred_element_type=jnp.float32
    )


def dot_nt(left, right):
    return lax.dot_general(
        left, right, (((1,), (1,)), ((), ())), preferred_element_type=jnp.float32
    )


def dot_tn(left, right):
    return lax.dot_general(
        left, right, (((0,), (0,)), ((), ())), preferred_element_type=jnp.float32
    )


def half_sums(values):
    lane = lax.broadcasted_iota(jnp.int32, values.shape, 1)
    total = jnp.zeros_like(values)
    for head in range(values.shape[1] // HEAD):
        inside = (lane // HEAD) == head
        part = jnp.sum(jnp.where(inside, values, 0.0), axis=1, keepdims=True)
        total = jnp.where(inside, part, total)
    return total


def unit_lower_inverse(below):
    size = below[0].shape[0]
    row = lax.broadcasted_iota(jnp.int32, (size, size), 0)
    column = lax.broadcasted_iota(jnp.int32, (size, size), 1)
    eye = jnp.where(row == column, 1.0, 0.0)
    width = 1
    inverse = None
    while width < size:
        corner = (
            (row // (2 * width) == column // (2 * width))
            & ((row // width) % 2 == 1)
            & ((column // width) % 2 == 0)
        )
        off = [jnp.where(corner, block, 0.0) for block in below]
        if inverse is None:
            inverse = [eye + block for block in off]
        else:
            narrow = [block.astype(jnp.bfloat16) for block in inverse]
            middle = [
                dot_nn(block.astype(jnp.bfloat16), right).astype(jnp.bfloat16)
                for block, right in zip(off, narrow)
            ]
            inverse = [
                whole + dot_nn(left, right)
                for whole, left, right in zip(inverse, narrow, middle)
            ]
        width *= 2
    return [block.astype(jnp.bfloat16) for block in inverse]


def mixer_kernel(q_ref, k_ref, v_ref, decay_ref, rate_ref, local_ref, query_ref, final_ref):
    rows, lanes = q_ref.shape
    heads = lanes // HEAD
    size = min(CHUNK, rows)
    chunks = rows // size
    row = lax.broadcasted_iota(jnp.int32, (size, 2 * size), 0)
    column = lax.broadcasted_iota(jnp.int32, (size, 2 * size), 1) % size
    strict = row > column
    upto = row >= column
    triangle = jnp.where(
        lax.broadcasted_iota(jnp.int32, (size, size), 0)
        >= lax.broadcasted_iota(jnp.int32, (size, size), 1),
        1.0,
        0.0,
    )
    keys = k_ref[...]
    unit = keys * lax.rsqrt(half_sums(keys * keys) + unit_eps)
    erase = -unit
    write = unit * rate_ref[...]
    bf16 = jnp.bfloat16
    per_chunk = []
    for chunk in range(chunks):
        span = slice(chunk * size, (chunk + 1) * size)
        log_decay = decay_ref[span, :]
        cumulative = lax.dot_general(
            triangle,
            log_decay,
            (((1,), (0,)), ((), ())),
            precision=highest,
            preferred_element_type=jnp.float32,
        )
        last = cumulative[size - 1 : size, :]
        middle = 0.5 * last
        fall = jnp.exp(cumulative - middle)
        fall_before = jnp.exp(cumulative - log_decay - middle)
        rise = jnp.exp(middle - cumulative)
        half_fade = jnp.exp(middle)
        e_row = fall_before * erase[span]
        q_row = fall * q_ref[span, :]
        w_row = rise * write[span]
        k_row = rise * keys[span]
        per_chunk.append(
            dict(
                left=jnp.concatenate([e_row, q_row], axis=0).astype(bf16),
                right=jnp.concatenate([w_row, k_row], axis=0).astype(bf16),
                start=jnp.concatenate([e_row * half_fade, q_row * half_fade], axis=0).astype(bf16),
                end=jnp.concatenate([w_row * half_fade, k_row * half_fade], axis=0).astype(bf16),
                fade=jnp.exp(last),
            )
        )
    tables = {}
    for chunk in range(chunks):
        for head in range(heads):
            at = slice(head * HEAD, (head + 1) * HEAD)
            tables[chunk, head] = dot_nt(
                per_chunk[chunk]["left"][:, at], per_chunk[chunk]["right"][:, at]
            )
    order = sorted(tables)
    erase_tables = {key: jnp.where(strict, tables[key][:size], 0.0) for key in order}
    query_tables = {key: jnp.where(upto, tables[key][size:], 0.0).astype(bf16) for key in order}
    inverses = dict(
        zip(order, unit_lower_inverse([erase_tables[key][:, :size] for key in order]))
    )
    pad = jnp.zeros((size, HEAD), jnp.float32)
    carried = [
        jnp.where(
            lax.broadcasted_iota(jnp.int32, (2 * HEAD, HEAD), 0)
            == lax.broadcasted_iota(jnp.int32, (2 * HEAD, HEAD), 1) + HEAD,
            1.0,
            0.0,
        )
        for _ in range(heads)
    ]
    for chunk in range(chunks):
        span = slice(chunk * size, (chunk + 1) * size)
        work = per_chunk[chunk]
        outs = []
        for head in range(heads):
            at = slice(head * HEAD, (head + 1) * HEAD)
            values = jnp.concatenate([v_ref[span, at], pad], axis=1)
            from_start = dot_nt(work["start"][:, at], carried[head].astype(bf16))
            right_side = from_start[:size] + dot_nn(
                erase_tables[chunk, head].astype(bf16),
                jnp.concatenate([jnp.zeros_like(values), values], axis=0).astype(bf16),
            )
            held = dot_nn(inverses[chunk, head], right_side.astype(bf16))
            both = jnp.concatenate([held, values], axis=0).astype(bf16)
            outs.append(from_start[size:] + dot_nn(query_tables[chunk, head], both))
            carried[head] = carried[head] * work["fade"][:, at] + dot_tn(both, work["end"][:, at])
        local_ref[span, :] = jnp.concatenate([out[:, :HEAD] for out in outs], axis=1)
        query_ref[span, :] = jnp.concatenate([out[:, HEAD:] for out in outs], axis=1).astype(bf16)
    final_ref[...] = jnp.concatenate(carried, axis=1).astype(bf16)[None]


def mixer_local(query, keys, values, log_decay, rate, interpret=False):
    rows, channels = query.shape
    lanes = min(PAIR * HEAD, channels)
    steps = channels // lanes
    block = pl.BlockSpec((rows, lanes), lambda i: (0, i))
    return pl.pallas_call(
        mixer_kernel,
        grid=(steps,),
        in_specs=[block] * 5,
        out_specs=[block, block, pl.BlockSpec((1, 2 * HEAD, lanes), lambda i: (i, 0, 0))],
        out_shape=[
            jax.ShapeDtypeStruct((rows, channels), jnp.float32),
            jax.ShapeDtypeStruct((rows, channels), jnp.bfloat16),
            jax.ShapeDtypeStruct((steps, 2 * HEAD, lanes), jnp.bfloat16),
        ],
        cost_estimate=pl.CostEstimate(
            flops=rows * channels * 4096, bytes_accessed=rows * channels * 26, transcendentals=0
        ),
        name="mixer_local",
        interpret=interpret,
    )(query, keys, values, log_decay, rate)


def finish_kernel(place_ref, maps_ref, local_ref, query_ref, gain_ref, out_ref):
    steps, double, lanes = maps_ref.shape[1:]
    heads = lanes // HEAD
    bf16 = jnp.bfloat16
    same = (
        lax.broadcasted_iota(jnp.int32, (lanes, lanes), 0) // HEAD
        == lax.broadcasted_iota(jnp.int32, (lanes, lanes), 1) // HEAD
    )

    def hop(k, states):
        after = []
        for step in range(steps):
            moved = maps_ref[k, step, HEAD:, :]
            square = jnp.where(same, jnp.concatenate([moved] * heads, axis=0), 0).astype(bf16)
            high = states[step].astype(bf16)
            low = (states[step] - high.astype(jnp.float32)).astype(bf16)
            after.append(
                dot_nn(high, square)
                + dot_nn(low, square)
                + maps_ref[k, step, :HEAD, :].astype(jnp.float32)
            )
        return tuple(after)

    states = lax.fori_loop(
        0, place_ref[0], hop, tuple(jnp.zeros((HEAD, lanes), jnp.float32) for _ in range(steps))
    )
    for step in range(steps):
        at = slice(step * lanes, (step + 1) * lanes)
        square = jnp.where(same, jnp.concatenate([states[step]] * heads, axis=0), 0.0).astype(bf16)
        outputs = local_ref[:, at] + dot_nt(query_ref[:, at], square)
        centered = outputs - half_sums(outputs) * (1.0 / HEAD)
        variance = half_sums(centered * centered) * (1.0 / HEAD)
        scaled = centered * lax.rsqrt(variance + group_eps)
        out_ref[:, at] = (scaled * gain_ref[:, at].astype(jnp.float32)).astype(bf16)


def mixer_finish(place, maps, local, query, gain, interpret=False):
    vmem = pl.BlockSpec(memory_space=pltpu.VMEM)
    return pl.pallas_call(
        finish_kernel,
        in_specs=[pl.BlockSpec(memory_space=pltpu.SMEM)] + [vmem] * 4,
        out_specs=vmem,
        out_shape=jax.ShapeDtypeStruct(local.shape, jnp.bfloat16),
        cost_estimate=pl.CostEstimate(
            flops=local.size * 2048, bytes_accessed=maps.size * 2, transcendentals=0
        ),
        name="mixer_finish",
        interpret=interpret,
    )(place, maps, local, query, gain)


def slot_positions(route_block, experts):
    flat_ids = route_block.reshape(-1)
    onehot = (flat_ids[:, None] == jnp.arange(experts, dtype=jnp.int32)[None, :]).astype(jnp.int32)
    earlier_count = jnp.cumsum(onehot, axis=0) - onehot
    return jnp.sum(earlier_count * onehot, axis=1).reshape(route_block.shape)


def per_device(
    mixer_input,
    mixer_gain,
    query_matrix,
    key_matrix,
    value_matrix,
    decay_down_factor,
    decay_up_factor,
    decay_bias_base,
    decay_shift,
    decay_spike,
    correction_rate_down,
    correction_rate_up,
    correction_rate_base,
    head_norm_gain,
    output_weight,
    feedforward_input,
    feedforward_gain,
    routed_expert_index,
    routed_expert_weight,
    expert_gate_weight,
    expert_up_weight,
    expert_down_weight,
    shared_gate_weight,
    shared_up_weight,
    shared_down_weight,
):
    tp_size = lax.axis_size("tp")
    ep_size = lax.axis_size("ep")
    normed_first = rms_rows(mixer_input, mixer_gain)
    (
        query_matrix_rows,
        key_matrix_rows,
        value_matrix_rows,
        logarithm_decay,
        learning,
    ) = mixer_channel_rows(
        normed_first,
        query_matrix,
        key_matrix,
        value_matrix,
        decay_down_factor,
        decay_up_factor,
        decay_bias_base,
        decay_shift,
        decay_spike,
        correction_rate_down,
        correction_rate_up,
        correction_rate_base,
    )
    local, query_map, final = mixer_local(
        query_matrix_rows, key_matrix_rows, value_matrix_rows, logarithm_decay, learning
    )
    maps = lax.all_gather(final, "ep")
    mixed_rows = mixer_finish(
        lax.axis_index("ep").reshape(1), maps, local, query_map, head_norm_gain[None]
    )
    mixed_a = lax.psum_scatter(
        jnp.dot(mixed_rows, output_weight, preferred_element_type=jnp.float32).astype(jnp.bfloat16),
        "tp",
        scatter_dimension=0,
        tiled=True,
    )
    own_count = feedforward_input.shape[0]
    local_count = expert_gate_weight.shape[0]
    experts = local_count * ep_size
    capacity = max(2, 3 * own_count * TOP // (2 * experts))
    normed_own = rms_rows(feedforward_input, feedforward_gain)
    model_width = normed_own.shape[1]
    group_rows = lax.all_gather(normed_own, "tp", axis=0, tiled=True)
    own_ids = lax.dynamic_slice_in_dim(
        routed_expert_index, lax.axis_index("tp") * own_count, own_count, 0
    )
    own_positions = slot_positions(own_ids, experts)
    zero_row = jnp.zeros((1, model_width), jnp.bfloat16)
    slot_index = own_ids * capacity + own_positions
    slot_table = jnp.full((experts * capacity,), own_count, jnp.int32)
    slot_table = slot_table.at[slot_index.reshape(-1)].set(
        jnp.broadcast_to(jnp.arange(own_count, dtype=jnp.int32)[:, None], slot_index.shape).reshape(
            -1
        )
    )
    padded = jnp.concatenate([normed_own, zero_row], axis=0)
    outgoing = padded[slot_table].reshape(experts, capacity, model_width)
    received = lax.all_to_all(outgoing, "ep", split_axis=0, concat_axis=0, tiled=True)
    arrived = lax.all_gather(received[None], "tp", axis=0, tiled=True)
    arrived = arrived.reshape(tp_size, ep_size, local_count, capacity, model_width)
    gate_out = jnp.einsum(
        "tgjcd,jdf->tgjcf", arrived, expert_gate_weight, preferred_element_type=jnp.float32
    )
    up_out = jnp.einsum(
        "tgjcd,jdf->tgjcf", arrived, expert_up_weight, preferred_element_type=jnp.float32
    )
    hidden = (jax.nn.silu(gate_out) * up_out).astype(jnp.bfloat16)
    shared_hidden = (
        jax.nn.silu(jnp.dot(group_rows, shared_gate_weight, preferred_element_type=jnp.float32))
        * jnp.dot(group_rows, shared_up_weight, preferred_element_type=jnp.float32)
    ).astype(jnp.bfloat16)
    shared_hidden = shared_hidden.reshape(tp_size, own_count, -1)
    routed_rows = ep_size * local_count * capacity
    block_rows = routed_rows + own_count
    block_total = lax.axis_size("tp") * block_rows // block_rows
    routed_part = jnp.einsum(
        "tgjcf,jfd->tgjcd", hidden, expert_down_weight, preferred_element_type=jnp.float32
    )
    shared_part = jnp.einsum(
        "tnf,fd->tnd", shared_hidden, shared_down_weight, preferred_element_type=jnp.float32
    )
    joined = jnp.concatenate(
        [routed_part.reshape(block_total, routed_rows, model_width), shared_part], axis=1
    )
    summed = lax.psum_scatter(
        joined.reshape(lax.axis_size("tp") * block_rows, model_width).astype(jnp.bfloat16),
        "tp",
        scatter_dimension=0,
        tiled=True,
    ).astype(jnp.float32)
    expert_out = (
        summed[:routed_rows]
        .astype(jnp.bfloat16)
        .reshape(ep_size, local_count * capacity, model_width)
    )
    returned = lax.all_to_all(expert_out, "ep", split_axis=0, concat_axis=0, tiled=True).reshape(
        experts * capacity, model_width
    )
    picked = returned[own_ids * capacity + own_positions]
    routed = jnp.einsum(
        "rk,rkd->rd", routed_expert_weight, picked.astype(jnp.float32), precision=highest
    )
    mixed_b = (routed + summed[routed_rows:]).astype(jnp.bfloat16)
    return (mixed_a, mixed_b)


def solution(mesh):
    in_specs = (
        P("ep", None),
        P(),
        P(None, "tp"),
        P(None, "tp"),
        P(None, "tp"),
        P(),
        P(None, "tp"),
        P("tp"),
        P("ep", "tp"),
        P("ep", "tp"),
        P(),
        P(None, "tp"),
        P("tp"),
        P("tp"),
        P("tp", None),
        P(("ep", "tp"), None),
        P(),
        P("ep", None),
        P(("ep", "tp"), None),
        P("ep", None, "tp"),
        P("ep", None, "tp"),
        P("ep", "tp", None),
        P(None, "tp"),
        P(None, "tp"),
        P("tp", None),
    )
    out_specs = (P(("ep", "tp"), None), P(("ep", "tp"), None))
    return jax.shard_map(
        per_device, mesh=mesh, in_specs=in_specs, out_specs=out_specs, check_vma=False
    )
```

```python
import functools

import jax
import jax.numpy as jnp
from jax import lax
from jax.experimental import pallas as pl
from jax.experimental.pallas import tpu as pltpu
from jax.sharding import PartitionSpec as P

HEAD = 64
TOP = 2
CHUNK = 64
PAIR = 2


highest = lax.Precision.HIGHEST
norm_eps = 1e-06
group_eps = 0.00064
unit_eps = 1e-06


def rms_rows(matrix, gain):
    values = matrix.astype(jnp.float32)
    scaled = values * lax.rsqrt(jnp.mean(values * values, axis=-1, keepdims=True) + norm_eps)
    return (scaled * gain.astype(jnp.float32)).astype(jnp.bfloat16)


def mixer_channel_rows(
    normed_rows,
    query_matrix,
    key_matrix,
    value_matrix,
    decay_down_factor,
    decay_up_factor,
    decay_bias_base,
    decay_shift,
    decay_spike,
    correction_rate_down,
    correction_rate_up,
    correction_rate_base,
):
    query_matrix_rows = jnp.dot(normed_rows, query_matrix, preferred_element_type=jnp.float32)
    key_matrix_rows = jnp.dot(normed_rows, key_matrix, preferred_element_type=jnp.float32)
    value_matrix_rows = jnp.dot(normed_rows, value_matrix, preferred_element_type=jnp.float32)
    decay_low = jnp.tanh(
        jnp.dot(normed_rows, decay_down_factor, preferred_element_type=jnp.float32)
    ).astype(jnp.bfloat16)
    decay_logits = (
        decay_bias_base
        + jnp.dot(decay_low, decay_up_factor, preferred_element_type=jnp.float32)
        + decay_shift
    )
    logarithm_decay = decay_spike - jnp.exp(-jax.nn.softplus(-decay_logits) - 0.5)
    iclr_low = jnp.dot(
        normed_rows, correction_rate_down, preferred_element_type=jnp.float32
    ).astype(jnp.bfloat16)
    learning = jax.nn.sigmoid(
        correction_rate_base
        + jnp.dot(iclr_low, correction_rate_up, preferred_element_type=jnp.float32)
    )
    return (query_matrix_rows, key_matrix_rows, value_matrix_rows, logarithm_decay, learning)


def dot_nn(left, right):
    return lax.dot_general(
        left, right, (((1,), (0,)), ((), ())), preferred_element_type=jnp.float32
    )


def dot_nt(left, right):
    return lax.dot_general(
        left, right, (((1,), (1,)), ((), ())), preferred_element_type=jnp.float32
    )


def dot_tn(left, right):
    return lax.dot_general(
        left, right, (((0,), (0,)), ((), ())), preferred_element_type=jnp.float32
    )


def half_sums(values):
    lane = lax.broadcasted_iota(jnp.int32, values.shape, 1)
    total = jnp.zeros_like(values)
    for head in range(values.shape[1] // HEAD):
        inside = (lane // HEAD) == head
        part = jnp.sum(jnp.where(inside, values, 0.0), axis=1, keepdims=True)
        total = jnp.where(inside, part, total)
    return total


def unit_lower_inverse(below):
    size = below[0].shape[0]
    row = lax.broadcasted_iota(jnp.int32, (size, size), 0)
    column = lax.broadcasted_iota(jnp.int32, (size, size), 1)
    eye = jnp.where(row == column, 1.0, 0.0)
    width = 1
    inverse = None
    while width < size:
        corner = (
            (row // (2 * width) == column // (2 * width))
            & ((row // width) % 2 == 1)
            & ((column // width) % 2 == 0)
        )
        off = [jnp.where(corner, block, 0.0) for block in below]
        if inverse is None:
            inverse = [eye + block for block in off]
        else:
            narrow = [block.astype(jnp.bfloat16) for block in inverse]
            middle = [
                dot_nn(block.astype(jnp.bfloat16), right).astype(jnp.bfloat16)
                for block, right in zip(off, narrow)
            ]
            inverse = [
                whole + dot_nn(left, right)
                for whole, left, right in zip(inverse, narrow, middle)
            ]
        width *= 2
    return [block.astype(jnp.bfloat16) for block in inverse]


def mixer_kernel(q_ref, k_ref, v_ref, decay_ref, rate_ref, local_ref, query_ref, final_ref):
    rows, lanes = q_ref.shape
    heads = lanes // HEAD
    size = min(CHUNK, rows)
    chunks = rows // size
    row = lax.broadcasted_iota(jnp.int32, (size, 2 * size), 0)
    column = lax.broadcasted_iota(jnp.int32, (size, 2 * size), 1) % size
    strict = row > column
    upto = row >= column
    triangle = jnp.where(
        lax.broadcasted_iota(jnp.int32, (size, size), 0)
        >= lax.broadcasted_iota(jnp.int32, (size, size), 1),
        1.0,
        0.0,
    )
    keys = k_ref[...]
    unit = keys * lax.rsqrt(half_sums(keys * keys) + unit_eps)
    erase = -unit
    write = unit * rate_ref[...]
    bf16 = jnp.bfloat16
    per_chunk = []
    for chunk in range(chunks):
        span = slice(chunk * size, (chunk + 1) * size)
        log_decay = decay_ref[span, :]
        cumulative = lax.dot_general(
            triangle,
            log_decay,
            (((1,), (0,)), ((), ())),
            precision=highest,
            preferred_element_type=jnp.float32,
        )
        last = cumulative[size - 1 : size, :]
        middle = 0.5 * last
        fall = jnp.exp(cumulative - middle)
        fall_before = jnp.exp(cumulative - log_decay - middle)
        rise = jnp.exp(middle - cumulative)
        half_fade = jnp.exp(middle)
        e_row = fall_before * erase[span]
        q_row = fall * q_ref[span, :]
        w_row = rise * write[span]
        k_row = rise * keys[span]
        per_chunk.append(
            dict(
                left=jnp.concatenate([e_row, q_row], axis=0).astype(bf16),
                right=jnp.concatenate([w_row, k_row], axis=0).astype(bf16),
                start=jnp.concatenate([e_row * half_fade, q_row * half_fade], axis=0).astype(bf16),
                end=jnp.concatenate([w_row * half_fade, k_row * half_fade], axis=0).astype(bf16),
                fade=jnp.exp(last),
            )
        )
    tables = {}
    for chunk in range(chunks):
        for head in range(heads):
            at = slice(head * HEAD, (head + 1) * HEAD)
            tables[chunk, head] = dot_nt(
                per_chunk[chunk]["left"][:, at], per_chunk[chunk]["right"][:, at]
            )
    order = sorted(tables)
    erase_tables = {key: jnp.where(strict, tables[key][:size], 0.0) for key in order}
    query_tables = {key: jnp.where(upto, tables[key][size:], 0.0).astype(bf16) for key in order}
    inverses = dict(
        zip(order, unit_lower_inverse([erase_tables[key][:, :size] for key in order]))
    )
    pad = jnp.zeros((size, HEAD), jnp.float32)
    carried = [
        jnp.where(
            lax.broadcasted_iota(jnp.int32, (2 * HEAD, HEAD), 0)
            == lax.broadcasted_iota(jnp.int32, (2 * HEAD, HEAD), 1) + HEAD,
            1.0,
            0.0,
        )
        for _ in range(heads)
    ]
    for chunk in range(chunks):
        span = slice(chunk * size, (chunk + 1) * size)
        work = per_chunk[chunk]
        outs = []
        for head in range(heads):
            at = slice(head * HEAD, (head + 1) * HEAD)
            values = jnp.concatenate([v_ref[span, at], pad], axis=1)
            from_start = dot_nt(work["start"][:, at], carried[head].astype(bf16))
            right_side = from_start[:size] + dot_nn(
                erase_tables[chunk, head].astype(bf16),
                jnp.concatenate([jnp.zeros_like(values), values], axis=0).astype(bf16),
            )
            held = dot_nn(inverses[chunk, head], right_side.astype(bf16))
            both = jnp.concatenate([held, values], axis=0).astype(bf16)
            outs.append(from_start[size:] + dot_nn(query_tables[chunk, head], both))
            carried[head] = carried[head] * work["fade"][:, at] + dot_tn(both, work["end"][:, at])
        local_ref[span, :] = jnp.concatenate([out[:, :HEAD] for out in outs], axis=1)
        query_ref[span, :] = jnp.concatenate([out[:, HEAD:] for out in outs], axis=1).astype(bf16)
    final_ref[...] = jnp.concatenate(carried, axis=1).astype(bf16)[None]


def mixer_local(query, keys, values, log_decay, rate, interpret=False):
    rows, channels = query.shape
    lanes = min(PAIR * HEAD, channels)
    steps = channels // lanes
    block = pl.BlockSpec((rows, lanes), lambda i: (0, i))
    return pl.pallas_call(
        mixer_kernel,
        grid=(steps,),
        in_specs=[block] * 5,
        out_specs=[block, block, pl.BlockSpec((1, 2 * HEAD, lanes), lambda i: (i, 0, 0))],
        out_shape=[
            jax.ShapeDtypeStruct((rows, channels), jnp.float32),
            jax.ShapeDtypeStruct((rows, channels), jnp.bfloat16),
            jax.ShapeDtypeStruct((steps, 2 * HEAD, lanes), jnp.bfloat16),
        ],
        cost_estimate=pl.CostEstimate(
            flops=rows * channels * 4096, bytes_accessed=rows * channels * 26, transcendentals=0
        ),
        name="mixer_local",
        interpret=interpret,
    )(query, keys, values, log_decay, rate)


def finish_kernel(
    size, own_ref, local_ref, query_ref, gain_ref, out_ref, maps_ref, send_sems, recv_sems
):
    steps, double, lanes = own_ref.shape
    heads = lanes // HEAD
    bf16 = jnp.bfloat16
    me = lax.axis_index("ep")
    barrier = pltpu.get_barrier_semaphore()
    for ahead in range(1, size):
        pl.semaphore_signal(
            barrier,
            inc=1,
            device_id={"ep": lax.rem(me + ahead, size)},
            device_id_type=pl.DeviceIdType.MESH,
        )
    pl.semaphore_wait(barrier, size - 1)

    def copy_of(ahead):
        return pltpu.make_async_remote_copy(
            src_ref=own_ref,
            dst_ref=maps_ref.at[ahead],
            send_sem=send_sems.at[ahead],
            recv_sem=recv_sems.at[ahead],
            device_id={"ep": lax.rem(me + ahead, size)},
            device_id_type=pl.DeviceIdType.MESH,
        )

    for ahead in range(1, size):

        @pl.when(me + ahead < size)
        def _():
            copy_of(ahead).start()

    for ahead in range(1, size):

        @pl.when(me >= ahead)
        def _():
            copy_of(ahead).wait_recv()

    same = (
        lax.broadcasted_iota(jnp.int32, (lanes, lanes), 0) // HEAD
        == lax.broadcasted_iota(jnp.int32, (lanes, lanes), 1) // HEAD
    )

    def hop(k, states):
        after = []
        for step in range(steps):
            moved = maps_ref[me - k, step, HEAD:, :]
            square = jnp.where(same, jnp.concatenate([moved] * heads, axis=0), 0).astype(bf16)
            high = states[step].astype(bf16)
            low = (states[step] - high.astype(jnp.float32)).astype(bf16)
            after.append(
                dot_nn(high, square)
                + dot_nn(low, square)
                + maps_ref[me - k, step, :HEAD, :].astype(jnp.float32)
            )
        return tuple(after)

    states = lax.fori_loop(
        0, me, hop, tuple(jnp.zeros((HEAD, lanes), jnp.float32) for _ in range(steps))
    )
    for step in range(steps):
        at = slice(step * lanes, (step + 1) * lanes)
        square = jnp.where(same, jnp.concatenate([states[step]] * heads, axis=0), 0.0).astype(bf16)
        outputs = local_ref[:, at] + dot_nt(query_ref[:, at], square)
        centered = outputs - half_sums(outputs) * (1.0 / HEAD)
        variance = half_sums(centered * centered) * (1.0 / HEAD)
        scaled = centered * lax.rsqrt(variance + group_eps)
        out_ref[:, at] = (scaled * gain_ref[:, at].astype(jnp.float32)).astype(bf16)

    for ahead in range(1, size):

        @pl.when(me + ahead < size)
        def _():
            copy_of(ahead).wait_send()


def mixer_finish(final, local, query, gain):
    size = lax.axis_size("ep")
    vmem = pl.BlockSpec(memory_space=pltpu.VMEM)
    return pl.pallas_call(
        functools.partial(finish_kernel, size),
        in_specs=[vmem] * 4,
        out_specs=vmem,
        out_shape=jax.ShapeDtypeStruct(local.shape, jnp.bfloat16),
        scratch_shapes=[
            pltpu.VMEM((size,) + final.shape, jnp.bfloat16),
            pltpu.SemaphoreType.DMA((size,)),
            pltpu.SemaphoreType.DMA((size,)),
        ],
        compiler_params=pltpu.CompilerParams(collective_id=0, has_side_effects=True),
        cost_estimate=pl.CostEstimate(
            flops=final.size * 4096, bytes_accessed=final.size * size * 16, transcendentals=0
        ),
        name="mixer_finish",
    )(final, local, query, gain)


def slot_choices(route_block, experts, capacity):
    own_count, top = route_block.shape
    slot = jnp.arange(experts * capacity, dtype=jnp.int32)[None, :]
    chosen = [route_block[:, k : k + 1] == slot // capacity for k in range(top)]
    either = chosen[0]
    for more in chosen[1:]:
        either = either | more
    earlier = jnp.tri(own_count, k=-1, dtype=jnp.bfloat16)
    position = jnp.dot(
        earlier, either.astype(jnp.bfloat16), preferred_element_type=jnp.float32
    ).astype(jnp.int32)
    here = position == slot % capacity
    return [choice & here for choice in chosen]


def per_device(
    mixer_input,
    mixer_gain,
    query_matrix,
    key_matrix,
    value_matrix,
    decay_down_factor,
    decay_up_factor,
    decay_bias_base,
    decay_shift,
    decay_spike,
    correction_rate_down,
    correction_rate_up,
    correction_rate_base,
    head_norm_gain,
    output_weight,
    feedforward_input,
    feedforward_gain,
    routed_expert_index,
    routed_expert_weight,
    expert_gate_weight,
    expert_up_weight,
    expert_down_weight,
    shared_gate_weight,
    shared_up_weight,
    shared_down_weight,
):
    tp_size = lax.axis_size("tp")
    ep_size = lax.axis_size("ep")
    normed_first = rms_rows(mixer_input, mixer_gain)
    (
        query_matrix_rows,
        key_matrix_rows,
        value_matrix_rows,
        logarithm_decay,
        learning,
    ) = mixer_channel_rows(
        normed_first,
        query_matrix,
        key_matrix,
        value_matrix,
        decay_down_factor,
        decay_up_factor,
        decay_bias_base,
        decay_shift,
        decay_spike,
        correction_rate_down,
        correction_rate_up,
        correction_rate_base,
    )
    local, query_map, final = mixer_local(
        query_matrix_rows, key_matrix_rows, value_matrix_rows, logarithm_decay, learning
    )
    own_count = feedforward_input.shape[0]
    local_count = expert_gate_weight.shape[0]
    experts = local_count * ep_size
    capacity = max(2, 3 * own_count * TOP // (2 * experts))
    normed_own = rms_rows(feedforward_input, feedforward_gain)
    model_width = normed_own.shape[1]
    group_rows = lax.all_gather(normed_own, "tp", axis=0, tiled=True)
    own_ids = lax.dynamic_slice_in_dim(
        routed_expert_index, lax.axis_index("tp") * own_count, own_count, 0
    )
    choices = slot_choices(own_ids, experts, capacity)
    taken = choices[0]
    weighted = jnp.where(choices[0], routed_expert_weight[:, :1], 0.0)
    for k in range(1, TOP):
        taken = taken | choices[k]
        weighted = weighted + jnp.where(choices[k], routed_expert_weight[:, k : k + 1], 0.0)
    outgoing = lax.dot_general(
        taken.astype(jnp.bfloat16),
        normed_own,
        (((0,), (0,)), ((), ())),
        preferred_element_type=jnp.float32,
    ).astype(jnp.bfloat16)
    peer_rows = local_count * capacity
    received = lax.all_to_all(
        outgoing.reshape(ep_size, peer_rows, model_width), "ep", split_axis=0, concat_axis=0, tiled=True
    ).reshape(ep_size * peer_rows, model_width)
    final, received = lax.optimization_barrier((final, received))
    mixed_rows = mixer_finish(final, local, query_map, head_norm_gain[None])
    mixed_share = jnp.dot(mixed_rows, output_weight, preferred_element_type=jnp.float32).astype(
        jnp.bfloat16
    )
    routed_rows = ep_size * peer_rows
    arrived = lax.all_gather(received, "tp", axis=0, tiled=True)
    arrived, mixed_share = lax.optimization_barrier((arrived, mixed_share))
    mixed_a = lax.psum_scatter(mixed_share, "tp", scatter_dimension=0, tiled=True)
    owner = (jnp.arange(tp_size * routed_rows, dtype=jnp.int32) % peer_rows // capacity)[:, None]
    gate_out = jnp.dot(arrived, expert_gate_weight[0], preferred_element_type=jnp.float32)
    up_out = jnp.dot(arrived, expert_up_weight[0], preferred_element_type=jnp.float32)
    for j in range(1, local_count):
        gate_out = jnp.where(
            owner == j,
            jnp.dot(arrived, expert_gate_weight[j], preferred_element_type=jnp.float32),
            gate_out,
        )
        up_out = jnp.where(
            owner == j,
            jnp.dot(arrived, expert_up_weight[j], preferred_element_type=jnp.float32),
            up_out,
        )
    hidden = (jax.nn.silu(gate_out) * up_out).astype(jnp.bfloat16)
    hidden = jnp.concatenate(
        [jnp.where(owner == j, hidden, jnp.zeros_like(hidden)) for j in range(local_count)], axis=1
    )
    shared_hidden = (
        jax.nn.silu(jnp.dot(group_rows, shared_gate_weight, preferred_element_type=jnp.float32))
        * jnp.dot(group_rows, shared_up_weight, preferred_element_type=jnp.float32)
    ).astype(jnp.bfloat16)
    shared_hidden = shared_hidden.reshape(tp_size, own_count, -1)
    block_rows = routed_rows + own_count
    down_matrix = expert_down_weight.reshape(-1, model_width)
    routed_part = jnp.dot(hidden, down_matrix, preferred_element_type=jnp.float32).astype(
        jnp.bfloat16
    )
    shared_part = jnp.einsum(
        "tnf,fd->tnd", shared_hidden, shared_down_weight, preferred_element_type=jnp.float32
    ).astype(jnp.bfloat16)
    joined = jnp.concatenate(
        [routed_part.reshape(tp_size, routed_rows, model_width), shared_part], axis=1
    )
    summed = lax.psum_scatter(
        joined.reshape(tp_size * block_rows, model_width), "tp", scatter_dimension=0, tiled=True
    )
    expert_out = summed[:routed_rows].reshape(ep_size, peer_rows, model_width)
    returned = lax.all_to_all(expert_out, "ep", split_axis=0, concat_axis=0, tiled=True).reshape(
        experts * capacity, model_width
    )
    routed = jnp.dot(weighted, returned.astype(jnp.float32), precision=lax.Precision.HIGH)
    summed = summed.astype(jnp.float32)
    mixed_b = (routed + summed[routed_rows:]).astype(jnp.bfloat16)
    return (mixed_a, mixed_b)


def solution(mesh):
    in_specs = (
        P("ep", None),
        P(),
        P(None, "tp"),
        P(None, "tp"),
        P(None, "tp"),
        P(),
        P(None, "tp"),
        P("tp"),
        P("ep", "tp"),
        P("ep", "tp"),
        P(),
        P(None, "tp"),
        P("tp"),
        P("tp"),
        P("tp", None),
        P(("ep", "tp"), None),
        P(),
        P("ep", None),
        P(("ep", "tp"), None),
        P("ep", None, "tp"),
        P("ep", None, "tp"),
        P("ep", "tp", None),
        P(None, "tp"),
        P(None, "tp"),
        P("tp", None),
    )
    out_specs = (P(("ep", "tp"), None), P(("ep", "tp"), None))
    return jax.shard_map(
        per_device, mesh=mesh, in_specs=in_specs, out_specs=out_specs, check_vma=False
    )
```

```python
import functools

import jax
import jax.numpy as jnp
from jax import lax
from jax.experimental import pallas as pl
from jax.experimental.pallas import tpu as pltpu
from jax.sharding import PartitionSpec as P

HEAD = 64
TOP = 2
CHUNK = 64
PAIR = 2


highest = lax.Precision.HIGHEST
norm_eps = 1e-06
group_eps = 0.00064
unit_eps = 1e-06


def rms_rows(matrix, gain):
    values = matrix.astype(jnp.float32)
    scaled = values * lax.rsqrt(jnp.mean(values * values, axis=-1, keepdims=True) + norm_eps)
    return (scaled * gain.astype(jnp.float32)).astype(jnp.bfloat16)


def mixer_channel_rows(
    normed_rows,
    query_matrix,
    key_matrix,
    value_matrix,
    decay_down_factor,
    decay_up_factor,
    decay_bias_base,
    decay_shift,
    decay_spike,
    correction_rate_down,
    correction_rate_up,
    correction_rate_base,
):
    query_matrix_rows = jnp.dot(normed_rows, query_matrix, preferred_element_type=jnp.float32)
    key_matrix_rows = jnp.dot(normed_rows, key_matrix, preferred_element_type=jnp.float32)
    value_matrix_rows = jnp.dot(normed_rows, value_matrix, preferred_element_type=jnp.float32)
    decay_low = jnp.tanh(
        jnp.dot(normed_rows, decay_down_factor, preferred_element_type=jnp.float32)
    ).astype(jnp.bfloat16)
    decay_logits = (
        decay_bias_base
        + jnp.dot(decay_low, decay_up_factor, preferred_element_type=jnp.float32)
        + decay_shift
    )
    logarithm_decay = decay_spike - jnp.exp(-jax.nn.softplus(-decay_logits) - 0.5)
    iclr_low = jnp.dot(
        normed_rows, correction_rate_down, preferred_element_type=jnp.float32
    ).astype(jnp.bfloat16)
    learning = jax.nn.sigmoid(
        correction_rate_base
        + jnp.dot(iclr_low, correction_rate_up, preferred_element_type=jnp.float32)
    )
    return (query_matrix_rows, key_matrix_rows, value_matrix_rows, logarithm_decay, learning)


def dot_nn(left, right):
    return lax.dot_general(
        left, right, (((1,), (0,)), ((), ())), preferred_element_type=jnp.float32
    )


def dot_nt(left, right):
    return lax.dot_general(
        left, right, (((1,), (1,)), ((), ())), preferred_element_type=jnp.float32
    )


def dot_tn(left, right):
    return lax.dot_general(
        left, right, (((0,), (0,)), ((), ())), preferred_element_type=jnp.float32
    )


def half_sums(values):
    lane = lax.broadcasted_iota(jnp.int32, values.shape, 1)
    total = jnp.zeros_like(values)
    for head in range(values.shape[1] // HEAD):
        inside = (lane // HEAD) == head
        part = jnp.sum(jnp.where(inside, values, 0.0), axis=1, keepdims=True)
        total = jnp.where(inside, part, total)
    return total


def unit_lower_inverse(below):
    size = below[0].shape[0]
    row = lax.broadcasted_iota(jnp.int32, (size, size), 0)
    column = lax.broadcasted_iota(jnp.int32, (size, size), 1)
    eye = jnp.where(row == column, 1.0, 0.0)
    width = 1
    inverse = None
    while width < size:
        corner = (
            (row // (2 * width) == column // (2 * width))
            & ((row // width) % 2 == 1)
            & ((column // width) % 2 == 0)
        )
        off = [jnp.where(corner, block, 0.0) for block in below]
        if inverse is None:
            inverse = [eye + block for block in off]
        else:
            narrow = [block.astype(jnp.bfloat16) for block in inverse]
            middle = [
                dot_nn(block.astype(jnp.bfloat16), right).astype(jnp.bfloat16)
                for block, right in zip(off, narrow)
            ]
            inverse = [
                whole + dot_nn(left, right)
                for whole, left, right in zip(inverse, narrow, middle)
            ]
        width *= 2
    return [block.astype(jnp.bfloat16) for block in inverse]


def mixer_kernel(q_ref, k_ref, v_ref, decay_ref, rate_ref, local_ref, query_ref, final_ref):
    rows, lanes = q_ref.shape
    heads = lanes // HEAD
    size = min(CHUNK, rows)
    chunks = rows // size
    row = lax.broadcasted_iota(jnp.int32, (size, 2 * size), 0)
    column = lax.broadcasted_iota(jnp.int32, (size, 2 * size), 1) % size
    strict = row > column
    upto = row >= column
    triangle = jnp.where(
        lax.broadcasted_iota(jnp.int32, (size, size), 0)
        >= lax.broadcasted_iota(jnp.int32, (size, size), 1),
        1.0,
        0.0,
    )
    keys = k_ref[...]
    unit = keys * lax.rsqrt(half_sums(keys * keys) + unit_eps)
    erase = -unit
    write = unit * rate_ref[...]
    bf16 = jnp.bfloat16
    per_chunk = []
    for chunk in range(chunks):
        span = slice(chunk * size, (chunk + 1) * size)
        log_decay = decay_ref[span, :]
        cumulative = lax.dot_general(
            triangle,
            log_decay,
            (((1,), (0,)), ((), ())),
            precision=highest,
            preferred_element_type=jnp.float32,
        )
        last = cumulative[size - 1 : size, :]
        middle = 0.5 * last
        fall = jnp.exp(cumulative - middle)
        fall_before = jnp.exp(cumulative - log_decay - middle)
        rise = jnp.exp(middle - cumulative)
        half_fade = jnp.exp(middle)
        e_row = fall_before * erase[span]
        q_row = fall * q_ref[span, :]
        w_row = rise * write[span]
        k_row = rise * keys[span]
        per_chunk.append(
            dict(
                left=jnp.concatenate([e_row, q_row], axis=0).astype(bf16),
                right=jnp.concatenate([w_row, k_row], axis=0).astype(bf16),
                start=jnp.concatenate([e_row * half_fade, q_row * half_fade], axis=0).astype(bf16),
                end=jnp.concatenate([w_row * half_fade, k_row * half_fade], axis=0).astype(bf16),
                fade=jnp.exp(last),
            )
        )
    tables = {}
    for chunk in range(chunks):
        for head in range(heads):
            at = slice(head * HEAD, (head + 1) * HEAD)
            tables[chunk, head] = dot_nt(
                per_chunk[chunk]["left"][:, at], per_chunk[chunk]["right"][:, at]
            )
    order = sorted(tables)
    erase_tables = {key: jnp.where(strict, tables[key][:size], 0.0) for key in order}
    query_tables = {key: jnp.where(upto, tables[key][size:], 0.0).astype(bf16) for key in order}
    inverses = dict(
        zip(order, unit_lower_inverse([erase_tables[key][:, :size] for key in order]))
    )
    pad = jnp.zeros((size, HEAD), jnp.float32)
    carried = [
        jnp.where(
            lax.broadcasted_iota(jnp.int32, (2 * HEAD, HEAD), 0)
            == lax.broadcasted_iota(jnp.int32, (2 * HEAD, HEAD), 1) + HEAD,
            1.0,
            0.0,
        )
        for _ in range(heads)
    ]
    for chunk in range(chunks):
        span = slice(chunk * size, (chunk + 1) * size)
        work = per_chunk[chunk]
        outs = []
        for head in range(heads):
            at = slice(head * HEAD, (head + 1) * HEAD)
            values = jnp.concatenate([v_ref[span, at], pad], axis=1)
            from_start = dot_nt(work["start"][:, at], carried[head].astype(bf16))
            right_side = from_start[:size] + dot_nn(
                erase_tables[chunk, head].astype(bf16),
                jnp.concatenate([jnp.zeros_like(values), values], axis=0).astype(bf16),
            )
            held = dot_nn(inverses[chunk, head], right_side.astype(bf16))
            both = jnp.concatenate([held, values], axis=0).astype(bf16)
            outs.append(from_start[size:] + dot_nn(query_tables[chunk, head], both))
            carried[head] = carried[head] * work["fade"][:, at] + dot_tn(both, work["end"][:, at])
        local_ref[span, :] = jnp.concatenate([out[:, :HEAD] for out in outs], axis=1)
        query_ref[span, :] = jnp.concatenate([out[:, HEAD:] for out in outs], axis=1).astype(bf16)
    final_ref[...] = jnp.concatenate(carried, axis=1).astype(bf16)[None]


def mixer_local(query, keys, values, log_decay, rate, interpret=False):
    rows, channels = query.shape
    lanes = min(PAIR * HEAD, channels)
    steps = channels // lanes
    block = pl.BlockSpec((rows, lanes), lambda i: (0, i))
    return pl.pallas_call(
        mixer_kernel,
        grid=(steps,),
        in_specs=[block] * 5,
        out_specs=[block, block, pl.BlockSpec((1, 2 * HEAD, lanes), lambda i: (i, 0, 0))],
        out_shape=[
            jax.ShapeDtypeStruct((rows, channels), jnp.float32),
            jax.ShapeDtypeStruct((rows, channels), jnp.bfloat16),
            jax.ShapeDtypeStruct((steps, 2 * HEAD, lanes), jnp.bfloat16),
        ],
        cost_estimate=pl.CostEstimate(
            flops=rows * channels * 4096, bytes_accessed=rows * channels * 26, transcendentals=0
        ),
        name="mixer_local",
        interpret=interpret,
    )(query, keys, values, log_decay, rate)


def finish_kernel(
    size, own_ref, local_ref, query_ref, gain_ref, out_ref, maps_ref, send_sems, recv_sems
):
    steps, double, lanes = own_ref.shape
    heads = lanes // HEAD
    bf16 = jnp.bfloat16
    me = lax.axis_index("ep")
    barrier = pltpu.get_barrier_semaphore()
    for ahead in range(1, size):
        pl.semaphore_signal(
            barrier,
            inc=1,
            device_id={"ep": lax.rem(me + ahead, size)},
            device_id_type=pl.DeviceIdType.MESH,
        )
    pl.semaphore_wait(barrier, size - 1)

    def copy_of(ahead):
        return pltpu.make_async_remote_copy(
            src_ref=own_ref,
            dst_ref=maps_ref.at[ahead],
            send_sem=send_sems.at[ahead],
            recv_sem=recv_sems.at[ahead],
            device_id={"ep": lax.rem(me + ahead, size)},
            device_id_type=pl.DeviceIdType.MESH,
        )

    for ahead in range(1, size):

        @pl.when(me + ahead < size)
        def _():
            copy_of(ahead).start()

    for ahead in range(1, size):

        @pl.when(me >= ahead)
        def _():
            copy_of(ahead).wait_recv()

    same = (
        lax.broadcasted_iota(jnp.int32, (lanes, lanes), 0) // HEAD
        == lax.broadcasted_iota(jnp.int32, (lanes, lanes), 1) // HEAD
    )

    def hop(k, states):
        after = []
        for step in range(steps):
            moved = maps_ref[me - k, step, HEAD:, :]
            square = jnp.where(same, jnp.concatenate([moved] * heads, axis=0), 0).astype(bf16)
            high = states[step].astype(bf16)
            low = (states[step] - high.astype(jnp.float32)).astype(bf16)
            after.append(
                dot_nn(high, square)
                + dot_nn(low, square)
                + maps_ref[me - k, step, :HEAD, :].astype(jnp.float32)
            )
        return tuple(after)

    states = lax.fori_loop(
        0, me, hop, tuple(jnp.zeros((HEAD, lanes), jnp.float32) for _ in range(steps))
    )
    for step in range(steps):
        at = slice(step * lanes, (step + 1) * lanes)
        square = jnp.where(same, jnp.concatenate([states[step]] * heads, axis=0), 0.0).astype(bf16)
        outputs = local_ref[:, at] + dot_nt(query_ref[:, at], square)
        centered = outputs - half_sums(outputs) * (1.0 / HEAD)
        variance = half_sums(centered * centered) * (1.0 / HEAD)
        scaled = centered * lax.rsqrt(variance + group_eps)
        out_ref[:, at] = (scaled * gain_ref[:, at].astype(jnp.float32)).astype(bf16)

    for ahead in range(1, size):

        @pl.when(me + ahead < size)
        def _():
            copy_of(ahead).wait_send()


def mixer_finish(final, local, query, gain):
    size = lax.axis_size("ep")
    vmem = pl.BlockSpec(memory_space=pltpu.VMEM)
    return pl.pallas_call(
        functools.partial(finish_kernel, size),
        in_specs=[vmem] * 4,
        out_specs=vmem,
        out_shape=jax.ShapeDtypeStruct(local.shape, jnp.bfloat16),
        scratch_shapes=[
            pltpu.VMEM((size,) + final.shape, jnp.bfloat16),
            pltpu.SemaphoreType.DMA((size,)),
            pltpu.SemaphoreType.DMA((size,)),
        ],
        compiler_params=pltpu.CompilerParams(collective_id=0, has_side_effects=True),
        cost_estimate=pl.CostEstimate(
            flops=final.size * 4096, bytes_accessed=final.size * size * 16, transcendentals=0
        ),
        name="mixer_finish",
    )(final, local, query, gain)


def halving_sum(shares, axis):
    size, me = lax.axis_size(axis), lax.axis_index(axis)
    distance = 1
    while distance < size:
        bit = (me // distance) % 2
        pairs = shares.reshape((shares.shape[0] // 2, 2) + shares.shape[1:])
        kept = lax.dynamic_index_in_dim(pairs, bit, 1, keepdims=False)
        given = lax.dynamic_index_in_dim(pairs, 1 - bit, 1, keepdims=False)
        came = lax.ppermute(given, axis, [(i, i ^ distance) for i in range(size)])
        shares = (kept.astype(jnp.float32) + came.astype(jnp.float32)).astype(jnp.bfloat16)
        distance *= 2
    return shares[0]


def slot_choices(route_block, experts, capacity):
    own_count, top = route_block.shape
    slot = jnp.arange(experts * capacity, dtype=jnp.int32)[None, :]
    chosen = [route_block[:, k : k + 1] == slot // capacity for k in range(top)]
    either = chosen[0]
    for more in chosen[1:]:
        either = either | more
    earlier = jnp.tri(own_count, k=-1, dtype=jnp.bfloat16)
    position = jnp.dot(
        earlier, either.astype(jnp.bfloat16), preferred_element_type=jnp.float32
    ).astype(jnp.int32)
    here = position == slot % capacity
    return [choice & here for choice in chosen]


def per_device(
    mixer_input,
    mixer_gain,
    query_matrix,
    key_matrix,
    value_matrix,
    decay_down_factor,
    decay_up_factor,
    decay_bias_base,
    decay_shift,
    decay_spike,
    correction_rate_down,
    correction_rate_up,
    correction_rate_base,
    head_norm_gain,
    output_weight,
    feedforward_input,
    feedforward_gain,
    routed_expert_index,
    routed_expert_weight,
    expert_gate_weight,
    expert_up_weight,
    expert_down_weight,
    shared_gate_weight,
    shared_up_weight,
    shared_down_weight,
):
    tp_size = lax.axis_size("tp")
    ep_size = lax.axis_size("ep")
    normed_first = rms_rows(mixer_input, mixer_gain)
    (
        query_matrix_rows,
        key_matrix_rows,
        value_matrix_rows,
        logarithm_decay,
        learning,
    ) = mixer_channel_rows(
        normed_first,
        query_matrix,
        key_matrix,
        value_matrix,
        decay_down_factor,
        decay_up_factor,
        decay_bias_base,
        decay_shift,
        decay_spike,
        correction_rate_down,
        correction_rate_up,
        correction_rate_base,
    )
    local, query_map, final = mixer_local(
        query_matrix_rows, key_matrix_rows, value_matrix_rows, logarithm_decay, learning
    )
    own_count = feedforward_input.shape[0]
    local_count = expert_gate_weight.shape[0]
    experts = local_count * ep_size
    capacity = max(2, 3 * own_count * TOP // (2 * experts))
    normed_own = rms_rows(feedforward_input, feedforward_gain)
    model_width = normed_own.shape[1]
    group_rows = lax.all_gather(normed_own, "tp", axis=0, tiled=True)
    own_ids = lax.dynamic_slice_in_dim(
        routed_expert_index, lax.axis_index("tp") * own_count, own_count, 0
    )
    choices = slot_choices(own_ids, experts, capacity)
    taken = choices[0]
    weighted = jnp.where(choices[0], routed_expert_weight[:, :1], 0.0)
    for k in range(1, TOP):
        taken = taken | choices[k]
        weighted = weighted + jnp.where(choices[k], routed_expert_weight[:, k : k + 1], 0.0)
    outgoing = lax.dot_general(
        taken.astype(jnp.bfloat16),
        normed_own,
        (((0,), (0,)), ((), ())),
        preferred_element_type=jnp.float32,
    ).astype(jnp.bfloat16)
    peer_rows = local_count * capacity
    received = lax.all_to_all(
        outgoing.reshape(ep_size, peer_rows, model_width), "ep", split_axis=0, concat_axis=0, tiled=True
    ).reshape(ep_size * peer_rows, model_width)
    final, received = lax.optimization_barrier((final, received))
    mixed_rows = mixer_finish(final, local, query_map, head_norm_gain[None])
    mixed_share = jnp.dot(mixed_rows, output_weight, preferred_element_type=jnp.float32).astype(
        jnp.bfloat16
    )
    routed_rows = ep_size * peer_rows
    arrived = lax.all_gather(received, "tp", axis=0, tiled=True)
    arrived, mixed_share = lax.optimization_barrier((arrived, mixed_share))
    mixed_a = halving_sum(mixed_share.reshape(tp_size, -1, model_width), "tp")
    owner = (jnp.arange(tp_size * routed_rows, dtype=jnp.int32) % peer_rows // capacity)[:, None]
    gate_out = jnp.dot(arrived, expert_gate_weight[0], preferred_element_type=jnp.float32)
    up_out = jnp.dot(arrived, expert_up_weight[0], preferred_element_type=jnp.float32)
    for j in range(1, local_count):
        gate_out = jnp.where(
            owner == j,
            jnp.dot(arrived, expert_gate_weight[j], preferred_element_type=jnp.float32),
            gate_out,
        )
        up_out = jnp.where(
            owner == j,
            jnp.dot(arrived, expert_up_weight[j], preferred_element_type=jnp.float32),
            up_out,
        )
    hidden = (jax.nn.silu(gate_out) * up_out).astype(jnp.bfloat16)
    hidden = jnp.concatenate(
        [jnp.where(owner == j, hidden, jnp.zeros_like(hidden)) for j in range(local_count)], axis=1
    )
    shared_hidden = (
        jax.nn.silu(jnp.dot(group_rows, shared_gate_weight, preferred_element_type=jnp.float32))
        * jnp.dot(group_rows, shared_up_weight, preferred_element_type=jnp.float32)
    ).astype(jnp.bfloat16)
    shared_hidden = shared_hidden.reshape(tp_size, own_count, -1)
    block_rows = routed_rows + own_count
    down_matrix = expert_down_weight.reshape(-1, model_width)
    routed_part = jnp.dot(hidden, down_matrix, preferred_element_type=jnp.float32).astype(
        jnp.bfloat16
    )
    shared_part = jnp.einsum(
        "tnf,fd->tnd", shared_hidden, shared_down_weight, preferred_element_type=jnp.float32
    ).astype(jnp.bfloat16)
    joined = jnp.concatenate(
        [routed_part.reshape(tp_size, routed_rows, model_width), shared_part], axis=1
    )
    summed = halving_sum(joined, "tp")
    expert_out = summed[:routed_rows].reshape(ep_size, peer_rows, model_width)
    returned = lax.all_to_all(expert_out, "ep", split_axis=0, concat_axis=0, tiled=True).reshape(
        experts * capacity, model_width
    )
    routed = jnp.dot(weighted, returned.astype(jnp.float32), precision=lax.Precision.HIGH)
    summed = summed.astype(jnp.float32)
    mixed_b = (routed + summed[routed_rows:]).astype(jnp.bfloat16)
    return (mixed_a, mixed_b)


def solution(mesh):
    in_specs = (
        P("ep", None),
        P(),
        P(None, "tp"),
        P(None, "tp"),
        P(None, "tp"),
        P(),
        P(None, "tp"),
        P("tp"),
        P("ep", "tp"),
        P("ep", "tp"),
        P(),
        P(None, "tp"),
        P("tp"),
        P("tp"),
        P("tp", None),
        P(("ep", "tp"), None),
        P(),
        P("ep", None),
        P(("ep", "tp"), None),
        P("ep", None, "tp"),
        P("ep", None, "tp"),
        P("ep", "tp", None),
        P(None, "tp"),
        P(None, "tp"),
        P("tp", None),
    )
    out_specs = (P(("ep", "tp"), None), P(("ep", "tp"), None))
    return jax.shard_map(
        per_device, mesh=mesh, in_specs=in_specs, out_specs=out_specs, check_vma=False
    )
```
